32 devices in a mesh: sp: 16 (over z, y, core), tp: 2 (over x).
Axes of the slice: x: 2, y: 2, z: 4, core: 2. Of those that a mesh axis runs over, the one named last changes fastest.
Arguments:
- tokens: bfloat16 [4096, 2048], P('sp', 'tp'), may hold values from -64 to 64
- input_norm_gain: float32 [2048], replicated, may hold values from 0.1 to 1.9
- attention_query_weight: bfloat16 [2048, 512], P(None, 'tp'), may hold values from -0.21875 to 0.21875
- attention_key_weight: bfloat16 [2048, 512], P(None, 'tp'), may hold values from -0.21875 to 0.21875
- attention_value_weight: bfloat16 [2048, 512], P(None, 'tp'), may hold values from -0.125 to 0.125
- attention_score_bias: float32 [8], P('tp'), may hold values from -18 to -7
- recurrence_query_weight: bfloat16 [2048, 1024], P(None, 'tp'), may hold values from -0.125 to 0.125
- forget_weight: bfloat16 [2048, 1024], P(None, 'tp'), may hold values from -0.125 to 0.125
- input_weight: bfloat16 [2048, 512], P(None, 'tp'), may hold values from -0.125 to 0.125
- output_gate_weight: bfloat16 [2048, 512], P(None, 'tp'), may hold values from -0.125 to 0.125
- forget_minimum: float32 [8, 128], P('tp'), may hold values from 0.9 to 1
- decay_spikes: float32 [4096, 8], P('sp', 'tp'), may hold values from -2.2 to 0
- head_norm_gain: float32 [64], replicated, may hold values from 0.1 to 1.9
- attention_output_weight: bfloat16 [512, 2048], P('tp'), may hold values from -0.25 to 0.25
- recurrence_output_weight: bfloat16 [512, 2048], P('tp'), may hold values from -0.25 to 0.25
Outputs:
- mixed: bfloat16 [4096, 2048], P('sp', 'tp')
The draws below stay inside these ranges and needn't reach their ends.
All inputs are finite; a program needn't handle non-finite values.
Results may differ from the reference program's by a relative error of at most 0.018.
Values may be sent and summed in bfloat16 or wider, within the bound.
A program may use at most 64 MiB of HBM per device.

```python
import jax
import jax.numpy as jnp
from jax import lax

D = 2048
SB_HEADS = 8
HEAD = 64
REC_HEADS = 8
REC_KEY = 128
REC_VAL = 64
TOK_DEV = 256
REC_SPAN = 64
TOKENS = 4096


def draw_tokens(key, part):
    streams = jax.random.split(jax.random.fold_in(key, 11), 3)
    column_rise = jnp.exp(jnp.log(4.0) * jnp.arange(D, dtype=jnp.float32) / D)
    column_rough = jnp.exp(jax.random.uniform(streams[0], (D,), jnp.float32, -0.35, 0.35))
    row_scale = jnp.exp(jax.random.uniform(streams[1], (TOKENS, 1), jnp.float32, -0.7, 0.7))
    noise_field = jnp.clip(jax.random.normal(streams[2], (TOKENS, D), jnp.float32), -5.0, 5.0)
    return (noise_field * row_scale * column_rise[None, :] * column_rough[None, :]).astype(jnp.bfloat16)


def draw_attention_score_bias(key, part):
    spread = jax.random.uniform(jax.random.fold_in(key, 23), (SB_HEADS,), jnp.float32, jnp.log(0.3), jnp.log(3.0))
    return spread - jnp.log(90.0 * TOKENS)


def draw_forget_minimum(key, part):
    streams = jax.random.split(jax.random.fold_in(key, 31), 3)
    ranking = jax.random.permutation(streams[0], REC_HEADS)
    slow_count = REC_HEADS // 2
    is_slow = (ranking < slow_count)[:, None]
    slow_gap = jnp.exp(jax.random.uniform(streams[1], (REC_HEADS, REC_KEY), jnp.float32, jnp.log(0.2), jnp.log(1.2))) / TOKENS
    fast_gap = jnp.exp(jax.random.uniform(streams[2], (REC_HEADS, REC_KEY), jnp.float32, jnp.log(0.04), jnp.log(0.1)))
    return 1.0 - jnp.where(is_slow, slow_gap, fast_gap)


def draw_decay_spikes(key, part):
    streams = jax.random.split(jax.random.fold_in(key, 47), 3)
    block_count = TOKENS // TOK_DEV
    block_rate = jnp.exp(jax.random.uniform(streams[0], (block_count, 1, REC_HEADS), jnp.float32, jnp.log(0.15), jnp.log(0.6))) / TOKENS
    steady = -jnp.broadcast_to(block_rate, (block_count, TOK_DEV, REC_HEADS)).reshape(TOKENS, REC_HEADS)
    places = jax.random.randint(streams[1], (3, REC_HEADS), 0, TOKENS)
    struck = jnp.arange(TOKENS, dtype=jnp.int32)[:, None, None] == places[None]
    depth = jnp.log(jax.random.uniform(streams[2], (3, REC_HEADS), jnp.float32, 0.5, 0.8))
    return steady + jnp.sum(jnp.where(struck, depth[None], 0.0), axis=1)


def steps_of(rng, shape, cuts, low, top_value):
    def one(dim, blocks):
        heights = jax.random.uniform(jax.random.fold_in(jax.random.fold_in(rng, 6), dim), (blocks,), jnp.float32, low / len(cuts), top_value / len(cuts))
        return jnp.repeat(jnp.exp(heights), shape[dim] // blocks).reshape((-1,) + (1,) * (len(shape) - dim - 1))

    gain = one(*cuts[0])
    for cut in cuts[1:]:
        gain = gain * one(*cut)
    return gain


def normal_values(rng, extent, scale, reach, cuts=(), kind=jnp.bfloat16):
    entries = jax.random.normal(rng, extent, jnp.float32) * scale
    if len(cuts) > 0:
        entries = steps_of(rng, extent, cuts, -0.22, 0.18) * entries
    return jnp.clip(entries, min=-reach, max=reach).astype(kind)


def setup_inputs(seed: int = 0) -> dict:
    arg_keys = jax.random.split(jax.random.key(seed), 16)
    return {
        "tokens": draw_tokens(jax.random.fold_in(arg_keys[15], 71), 0),
        "input_norm_gain": jnp.clip(1.0 + 0.18 * jax.random.normal(arg_keys[1], (D,), jnp.float32), 0.1, 1.9),
        "attention_query_weight": normal_values(arg_keys[2], (D, SB_HEADS * HEAD), (D // 3) ** -0.5, 0.21875, ((1, 2),)),
        "attention_key_weight": normal_values(arg_keys[3], (D, SB_HEADS * HEAD), (D // 3) ** -0.5, 0.21875, ((1, 2),)),
        "attention_value_weight": normal_values(arg_keys[4], (D, SB_HEADS * HEAD), D ** -0.5, 0.125, ((1, 2),)),
        "attention_score_bias": draw_attention_score_bias(jax.random.fold_in(arg_keys[15], 71), 0),
        "recurrence_query_weight": normal_values(arg_keys[6], (D, REC_HEADS * REC_KEY), D ** -0.5, 0.125, ((1, 2),)),
        "forget_weight": normal_values(arg_keys[7], (D, REC_HEADS * REC_KEY), D ** -0.5, 0.125, ((1, 2),)),
        "input_weight": normal_values(arg_keys[8], (D, REC_HEADS * REC_VAL), D ** -0.5, 0.125, ((1, 2),)),
        "output_gate_weight": normal_values(arg_keys[9], (D, REC_HEADS * REC_VAL), D ** -0.5, 0.125, ((1, 2),)),
        "forget_minimum": draw_forget_minimum(jax.random.fold_in(arg_keys[15], 71), 0),
        "decay_spikes": draw_decay_spikes(jax.random.fold_in(arg_keys[15], 71), 0),
        "head_norm_gain": jnp.clip(1.0 + 0.18 * jax.random.normal(arg_keys[12], (REC_VAL,), jnp.float32), 0.1, 1.9),
        "attention_output_weight": normal_values(arg_keys[13], (SB_HEADS * HEAD, D), (SB_HEADS * HEAD) ** -0.5, 0.25, ((0, 2),)),
        "recurrence_output_weight": normal_values(arg_keys[14], (REC_HEADS * REC_VAL, D), (REC_HEADS * REC_VAL) ** -0.5, 0.25, ((0, 2),)),
    }


epsilon = 1e-06

def project(scaled, inverse, weight):
    return (jnp.dot(scaled, weight, preferred_element_type=jnp.float32) * inverse).astype(jnp.bfloat16)

def stick_breaking(query_stick, key_stick, value_stick, attention_score_bias):
    block_count = TOKENS // TOK_DEV
    query_blocks = query_stick.reshape(block_count, TOK_DEV, SB_HEADS, HEAD)
    key_heads = key_stick.reshape(TOKENS, SB_HEADS, HEAD).astype(jnp.float32)
    value_heads = value_stick.reshape(TOKENS, SB_HEADS, HEAD).astype(jnp.float32)
    key_pos = jnp.arange(TOKENS, dtype=jnp.int32)

    def one_block(inputs):
        query_block, number = inputs
        query_pos = number * TOK_DEV + jnp.arange(TOK_DEV, dtype=jnp.int32)
        scores = jnp.einsum('qhd,khd->hqk', query_block.astype(jnp.float32), key_heads) * HEAD ** (-0.5)
        scores = scores + attention_score_bias[:, None, None]
        before = (key_pos[None, :] < query_pos[:, None])[None]
        log_rest = jnp.where(before, jax.nn.log_sigmoid(-scores), 0.0)
        later_sum = lax.cumsum(log_rest, axis=2, reverse=True) - log_rest
        weights = jnp.where(before, jnp.exp(jax.nn.log_sigmoid(scores) + later_sum), 0.0).astype(jnp.bfloat16)
        final_output = jnp.einsum('hqk,khd->qhd', weights.astype(jnp.float32), value_heads)
        return final_output.reshape(TOK_DEV, SB_HEADS * HEAD).astype(jnp.bfloat16)
    blocks = lax.map(one_block, (query_blocks, jnp.arange(block_count, dtype=jnp.int32)))
    return blocks.reshape(TOKENS, SB_HEADS * HEAD)

def linear_recurrence(query_rows, forget_rows, input_rows, gate_rows, forget_minimum, decay_spikes, head_norm_gain):
    peak_value = lax.Precision.HIGHEST
    raised_values = jax.nn.silu(query_rows.astype(jnp.float32)).reshape(TOKENS, REC_HEADS, REC_KEY)
    admitted_input = (1.0 - forget_minimum)[None] * jax.nn.sigmoid(-forget_rows.astype(jnp.float32).reshape(TOKENS, REC_HEADS, REC_KEY))
    forget_logarithm = jnp.log1p(-admitted_input) + decay_spikes[:, :, None]
    inputs = input_rows.astype(jnp.float32).reshape(TOKENS, REC_HEADS, REC_VAL)
    span_count = TOKENS // REC_SPAN
    causal = jnp.tril(jnp.ones((REC_SPAN, REC_SPAN), jnp.bool_))[:, :, None, None]

    def to_spans(array):
        return array.reshape(span_count, REC_SPAN, REC_HEADS, array.shape[-1])

    def advance(recurrent_memory, pieces):
        window_query, window_admitted, window_input, span_log = pieces
        running_total = jnp.cumsum(span_log, axis=0)
        log_gaps = running_total[:, None] - running_total[None, :]
        decay_table = jnp.where(causal, jnp.exp(jnp.where(causal, log_gaps, 0.0)), 0.0)
        inner_scores = jnp.einsum('thk,shk,tshk->hts', window_query, window_admitted, decay_table, precision=peak_value)
        final_output = jnp.einsum('hts,shv->thv', inner_scores, window_input, precision=peak_value)
        final_output = final_output + jnp.einsum('zbg,bgp->zbp', window_query * jnp.exp(running_total), recurrent_memory, precision=peak_value)
        window_total = running_total[-1]
        recurrent_memory = recurrent_memory * jnp.exp(window_total)[:, :, None] + jnp.einsum('rof,roi->ofi', window_admitted * jnp.exp(window_total[None] - running_total), window_input, precision=peak_value)
        return (recurrent_memory, final_output)
    start_memory = jnp.zeros((REC_HEADS, REC_KEY, REC_VAL), jnp.float32)
    memory_end, outputs = lax.scan(advance, start_memory, (to_spans(raised_values), to_spans(admitted_input), to_spans(inputs), to_spans(forget_logarithm)))
    outputs = outputs.reshape(TOKENS, REC_HEADS, REC_VAL)
    normed = outputs * lax.rsqrt(lax.optimization_barrier(jnp.mean(outputs * outputs, axis=2, keepdims=True)) + epsilon) * head_norm_gain
    gated_out = normed * jax.nn.silu(gate_rows.astype(jnp.float32).reshape(TOKENS, REC_HEADS, REC_VAL))
    return gated_out.reshape(TOKENS, REC_HEADS * REC_VAL).astype(jnp.bfloat16)

def reference(tokens, input_norm_gain, attention_query_weight, attention_key_weight, attention_value_weight, attention_score_bias, recurrence_query_weight, forget_weight, input_weight, output_gate_weight, forget_minimum, decay_spikes, head_norm_gain, attention_output_weight, recurrence_output_weight):
    values = tokens.astype(jnp.float32)
    scaled = (values * input_norm_gain[None, :]).astype(jnp.bfloat16)
    inverse = lax.rsqrt(lax.optimization_barrier(jnp.mean(values * values, axis=1, keepdims=True)) + epsilon)
    query_stick = project(scaled, inverse, attention_query_weight)
    key_stick = project(scaled, inverse, attention_key_weight)
    value_stick = project(scaled, inverse, attention_value_weight)
    query_rows = project(scaled, inverse, recurrence_query_weight)
    forget_rows = project(scaled, inverse, forget_weight)
    input_rows = project(scaled, inverse, input_weight)
    gate_rows = project(scaled, inverse, output_gate_weight)
    stick_heads = stick_breaking(query_stick, key_stick, value_stick, attention_score_bias)
    recurrence_heads = linear_recurrence(query_rows, forget_rows, input_rows, gate_rows, forget_minimum, decay_spikes, head_norm_gain)
    mixed_out = jnp.dot(stick_heads, attention_output_weight, preferred_element_type=jnp.float32)
    mixed_out = mixed_out + jnp.dot(recurrence_heads, recurrence_output_weight, preferred_element_type=jnp.float32)
    return mixed_out.astype(jnp.bfloat16)
```

```python
import functools

import jax
import jax.numpy as jnp
from jax import lax
from jax.experimental import pallas as pl
from jax.experimental.pallas import tpu as pltpu
from jax.sharding import PartitionSpec as P

HEAD = 64
REC_KEY = 128
REC_VAL = 64
epsilon = 1e-06
VMEM = pl.BlockSpec(memory_space=pltpu.VMEM)
SMEM = pl.BlockSpec(memory_space=pltpu.SMEM)
NT = (((1,), (1,)), ((), ()))
TN = (((0,), (0,)), ((), ()))


def mm(a, b, dims=(((1,), (0,)), ((), ()))):
    return lax.dot_general(a, b, dims, preferred_element_type=jnp.float32)


def split(x):
    hi = x.astype(jnp.bfloat16)
    return hi, (x - hi.astype(jnp.float32)).astype(jnp.bfloat16)


def iota(shape, dim):
    return lax.broadcasted_iota(jnp.int32, shape, dim)


def local_kernel(q_ref, f_ref, v_ref, low_ref, spike_ref, spike_t_ref, out_ref, qdec_ref, state_ref):
    rows = q_ref.shape[0]
    heads = v_ref.shape[1] // REC_VAL
    r, c = iota((rows, rows), 0), iota((rows, rows), 1)
    causal = r >= c
    lower = causal.astype(jnp.bfloat16)
    upper = (r <= c).astype(jnp.bfloat16)
    hi, lo = split(spike_ref[...])
    spike_col = mm(lower, hi) + mm(lower, lo)
    hi, lo = split(spike_t_ref[...])
    spike_row = mm(hi, upper) + mm(lo, upper)
    for h in range(heads):
        ks = slice(h * REC_KEY, (h + 1) * REC_KEY)
        vs = slice(h * REC_VAL, (h + 1) * REC_VAL)
        q = q_ref[:, ks].astype(jnp.float32)
        lifted = q * jax.nn.sigmoid(q)
        intake = (1.0 - low_ref[:, ks]) * jax.nn.sigmoid(-f_ref[:, ks].astype(jnp.float32))
        hi, lo = split(jnp.log1p(-intake))
        run = mm(lower, hi) + mm(lower, lo)
        s_col = spike_col[:, h : h + 1]
        s_row = spike_row[h : h + 1, :]
        q_up = lifted * jnp.exp(run)
        k_down = (intake * jnp.exp(-run)).astype(jnp.bfloat16)
        decay = jnp.exp(jnp.where(causal, s_col - s_row, 0.0))
        inner = jnp.where(causal, mm(q_up.astype(jnp.bfloat16), k_down, NT) * decay, 0.0)
        v = v_ref[:, vs]
        out_ref[:, vs] = mm(inner.astype(jnp.bfloat16), v)
        qdec_ref[:, ks] = (q_up * jnp.exp(s_col)).astype(jnp.bfloat16)
        total = run[rows - 1 : rows, :] + s_col[rows - 1 : rows, :]
        k_end = (intake * jnp.exp(total - (run + s_col))).astype(jnp.bfloat16)
        state_ref[0:REC_VAL, ks] = mm(v, k_end, TN)
        state_ref[REC_VAL:, ks] = jnp.broadcast_to(total, (8, REC_KEY))


def mix_kernel(bias_ref, q_ref, kv_ref, local_ref, qdec_ref, gate_ref, gain_ref, states_ref, out_ref, acc, carry, state):
    rows, width = q_ref.shape
    heads = width // HEAD
    place = lax.axis_index("sp")
    r, c = iota((rows, rows), 0), iota((rows, rows), 1)
    before = c < r
    sums = jnp.concatenate(
        [(r > c).astype(jnp.bfloat16), jnp.ones((rows, 128), jnp.bfloat16)], axis=1
    )

    def block(number, first):
        for h in range(heads):
            hs = slice(h * HEAD, (h + 1) * HEAD)
            k = kv_ref[number, :, hs]
            v = kv_ref[number, :, width + h * HEAD : width + (h + 1) * HEAD]
            s = mm(q_ref[:, hs] * jnp.bfloat16(HEAD**-0.5), k, NT) + bias_ref[h]
            t = jnp.exp(-jnp.abs(s))
            soft = jnp.where(t < 3.5e-4, t, jnp.log(1.0 + t))
            log_sig = jnp.minimum(s, 0.0) - soft
            rest = log_sig - s
            if first:
                rest = jnp.where(before, rest, 0.0)
            both = mm(rest.astype(jnp.bfloat16), sums)
            later = both[:, :rows]
            if not first:
                later = later + jnp.concatenate([carry[h]] * (rows // 128), axis=1)
            w = jnp.exp(log_sig + later)
            if first:
                w = jnp.where(before, w, 0.0)
            o = mm(w.astype(jnp.bfloat16), v)
            if first:
                acc[:, hs] = o
                carry[h] = both[:, rows:]
            else:
                acc[:, hs] += o
                carry[h] += both[:, rows:]

    block(place, True)

    @pl.loop(0, place)
    def _(step):
        block(place - 1 - step, False)

    out_ref[:, :width] = acc[...].astype(jnp.bfloat16)

    state[...] = jnp.zeros_like(state)

    def earlier(step, suffix):
        number = place - 1 - step
        state[...] += states_ref[number, :REC_VAL, :] * jnp.exp(suffix)
        return suffix + states_ref[number, REC_VAL : REC_VAL + 1, :]

    lax.fori_loop(0, place, earlier, jnp.zeros((1, state.shape[1]), jnp.float32))
    for h in range(local_ref.shape[1] // REC_VAL):
        ks = slice(h * REC_KEY, (h + 1) * REC_KEY)
        vs = slice(h * REC_VAL, (h + 1) * REC_VAL)
        raw = local_ref[:, vs] + mm(qdec_ref[:, ks], state[:, ks].astype(jnp.bfloat16), NT)
        gate = gate_ref[:, vs].astype(jnp.float32)
        mean = jnp.sum(raw * raw, axis=1, keepdims=True) * (1.0 / REC_VAL)
        done = raw * lax.rsqrt(mean + epsilon) * gain_ref[...] * (gate * jax.nn.sigmoid(gate))
        out_ref[:, width + h * REC_VAL : width + (h + 1) * REC_VAL] = done.astype(jnp.bfloat16)


def shards(
    tp,
    tokens,
    input_norm_gain,
    attention_query_weight,
    attention_key_weight,
    attention_value_weight,
    attention_score_bias,
    recurrence_query_weight,
    forget_weight,
    input_weight,
    output_gate_weight,
    forget_minimum,
    decay_spikes,
    head_norm_gain,
    attention_output_weight,
    recurrence_output_weight,
):
    rows = tokens.shape[0]
    mine = lax.axis_index("tp")
    own_rows = jnp.concatenate([attention_output_weight, recurrence_output_weight], axis=0)
    columns = own_rows.shape[1] // tp

    def to_partner(array, shift):
        return lax.ppermute(array, "tp", [(i, (i + shift) % tp) for i in range(tp)])

    def cut(shift):
        return lax.dynamic_slice_in_dim(own_rows, lax.rem(mine + shift, tp) * columns, columns, 1)

    out_weights = [cut(0)] + [to_partner(cut(shift), shift) for shift in range(1, tp)]

    values = lax.all_gather(tokens, "tp", axis=1, tiled=True).astype(jnp.float32)
    scaled = (values * input_norm_gain[None, :]).astype(jnp.bfloat16)
    squares = jnp.mean(values * values, axis=1)
    inverse = lax.rsqrt(squares + epsilon)[:, None]

    def project(weight):
        return (jnp.dot(scaled, weight, preferred_element_type=jnp.float32) * inverse).astype(jnp.bfloat16)

    key_stick, value_stick = project(attention_key_weight), project(attention_value_weight)
    kv_all = lax.all_gather(jnp.concatenate([key_stick, value_stick], axis=1), "sp")
    query_rows, forget_rows = project(recurrence_query_weight), project(forget_weight)
    input_rows = project(input_weight)
    heads_here = forget_minimum.shape[0]
    wide, narrow = heads_here * REC_KEY, heads_here * REC_VAL
    local_out, query_decayed, state_here = pl.pallas_call(
        local_kernel,
        out_shape=(
            jax.ShapeDtypeStruct((rows, narrow), jnp.float32),
            jax.ShapeDtypeStruct((rows, wide), jnp.bfloat16),
            jax.ShapeDtypeStruct((REC_VAL + 8, wide), jnp.float32),
        ),
        in_specs=[VMEM] * 6,
        out_specs=(VMEM,) * 3,
        cost_estimate=pl.CostEstimate(flops=10**9, bytes_accessed=2 * 10**6, transcendentals=10**6),
        name="recurrence_local",
    )(
        query_rows,
        forget_rows,
        input_rows,
        forget_minimum.reshape(1, wide),
        decay_spikes,
        decay_spikes.T,
    )
    states = lax.all_gather(state_here, "sp")
    query_stick, gate_rows = project(attention_query_weight), project(output_gate_weight)
    width = query_stick.shape[1]
    heads = pl.pallas_call(
        mix_kernel,
        out_shape=jax.ShapeDtypeStruct((rows, width + narrow), jnp.bfloat16),
        in_specs=[SMEM] + [VMEM] * 7,
        out_specs=VMEM,
        scratch_shapes=[
            pltpu.VMEM((rows, width), jnp.float32),
            pltpu.VMEM((width // HEAD, rows, 128), jnp.float32),
            pltpu.VMEM((REC_VAL, wide), jnp.float32),
        ],
        compiler_params=pltpu.CompilerParams(vmem_limit_bytes=60 * 1024 * 1024),
        name="mix_heads",
    )(
        attention_score_bias,
        query_stick,
        kv_all,
        local_out,
        query_decayed,
        gate_rows,
        head_norm_gain.reshape(1, REC_VAL),
        states,
    )
    mixed = jnp.dot(heads, out_weights[0], preferred_element_type=jnp.float32)
    for shift in range(1, tp):
        mixed = mixed + jnp.dot(to_partner(heads, shift), out_weights[shift], preferred_element_type=jnp.float32)
    return mixed.astype(jnp.bfloat16)


def solution(mesh):
    placed = (
        P("sp", "tp"),
        P(),
        P(None, "tp"),
        P(None, "tp"),
        P(None, "tp"),
        P("tp"),
        P(None, "tp"),
        P(None, "tp"),
        P(None, "tp"),
        P(None, "tp"),
        P("tp", None),
        P("sp", "tp"),
        P(),
        P("tp", None),
        P("tp", None),
    )
    return jax.shard_map(
        functools.partial(shards, mesh.shape["tp"]),
        mesh=mesh,
        in_specs=placed,
        out_specs=P("sp", "tp"),
        check_vma=False,
    )
```

```python
import functools

import jax
import jax.numpy as jnp
from jax import lax
from jax.experimental import pallas as pl
from jax.experimental.pallas import tpu as pltpu
from jax.sharding import PartitionSpec as P

HEAD = 64
REC_KEY = 128
REC_VAL = 64
TAIL = 16
epsilon = 1e-06
VMEM = pl.BlockSpec(memory_space=pltpu.VMEM)
SMEM = pl.BlockSpec(memory_space=pltpu.SMEM)
NT = (((1,), (1,)), ((), ()))
TN = (((0,), (0,)), ((), ()))


def mm(a, b, dims=(((1,), (0,)), ((), ()))):
    return lax.dot_general(a, b, dims, preferred_element_type=jnp.float32)


def split(x):
    hi = x.astype(jnp.bfloat16)
    return hi, (x - hi.astype(jnp.float32)).astype(jnp.bfloat16)


def iota(shape, dim):
    return lax.broadcasted_iota(jnp.int32, shape, dim)


def local_kernel(
    key_ref, value_ref, q_ref, f_ref, v_ref, low_ref, spike_ref, spike_t_ref, out_ref, qdec_ref, pay_ref
):
    rows, width = key_ref.shape
    pay_ref[0:rows, :width] = key_ref[...]
    pay_ref[0:rows, width:] = value_ref[...]
    which = iota((TAIL, REC_KEY), 0)
    heads = v_ref.shape[1] // REC_VAL
    r, c = iota((rows, rows), 0), iota((rows, rows), 1)
    causal = r >= c
    lower = causal.astype(jnp.bfloat16)
    upper = (r <= c).astype(jnp.bfloat16)
    hi, lo = split(spike_ref[...])
    spike_col = mm(lower, hi) + mm(lower, lo)
    hi, lo = split(spike_t_ref[...])
    spike_row = mm(hi, upper) + mm(lo, upper)
    for h in range(heads):
        ks = slice(h * REC_KEY, (h + 1) * REC_KEY)
        vs = slice(h * REC_VAL, (h + 1) * REC_VAL)
        q = q_ref[:, ks].astype(jnp.float32)
        lifted = q * jax.nn.sigmoid(q)
        intake = (1.0 - low_ref[:, ks]) * jax.nn.sigmoid(-f_ref[:, ks].astype(jnp.float32))
        hi, lo = split(jnp.log1p(-intake))
        run = mm(lower, hi) + mm(lower, lo)
        s_col = spike_col[:, h : h + 1]
        s_row = spike_row[h : h + 1, :]
        q_up = lifted * jnp.exp(run)
        k_down = (intake * jnp.exp(-run)).astype(jnp.bfloat16)
        decay = jnp.exp(jnp.where(causal, s_col - s_row, 0.0))
        inner = jnp.where(causal, mm(q_up.astype(jnp.bfloat16), k_down, NT) * decay, 0.0)
        v = v_ref[:, vs]
        out_ref[:, vs] = mm(inner.astype(jnp.bfloat16), v)
        qdec_ref[:, ks] = (q_up * jnp.exp(s_col)).astype(jnp.bfloat16)
        total = run[rows - 1 : rows, :] + s_col[rows - 1 : rows, :]
        k_end = (intake * jnp.exp(total - (run + s_col))).astype(jnp.bfloat16)
        pay_ref[rows : rows + REC_VAL, ks] = mm(v, k_end, TN).astype(jnp.bfloat16)
        hi, lo = split(total)
        lo, rest = split(total - hi.astype(jnp.float32))
        tail = jnp.where(which == 0, hi.astype(jnp.float32), jnp.where(which == 1, lo.astype(jnp.float32), 0.0))
        tail = jnp.where(which == 2, rest.astype(jnp.float32), tail)
        pay_ref[rows + REC_VAL :, ks] = tail.astype(jnp.bfloat16)


def mix_kernel(bias_ref, q_ref, kv_ref, local_ref, qdec_ref, gate_ref, gain_ref, out_ref, acc, carry, state):
    rows, width = q_ref.shape
    heads = width // HEAD
    place = lax.axis_index("sp")
    r, c = iota((rows, rows), 0), iota((rows, rows), 1)
    before = c < r
    sums = jnp.concatenate(
        [(r > c).astype(jnp.bfloat16), jnp.ones((rows, 128), jnp.bfloat16)], axis=1
    )

    def block(number, first):
        for h in range(heads):
            hs = slice(h * HEAD, (h + 1) * HEAD)
            k = kv_ref[number, :rows, hs]
            v = kv_ref[number, :rows, width + h * HEAD : width + (h + 1) * HEAD]
            s = mm(q_ref[:, hs] * jnp.bfloat16(HEAD**-0.5), k, NT) + bias_ref[h]
            t = jnp.exp(-jnp.abs(s))
            soft = jnp.where(t < 3.5e-4, t, jnp.log(1.0 + t))
            log_sig = jnp.minimum(s, 0.0) - soft
            rest = log_sig - s
            if first:
                rest = jnp.where(before, rest, 0.0)
            both = mm(rest.astype(jnp.bfloat16), sums)
            later = both[:, :rows]
            if not first:
                later = later + jnp.concatenate([carry[h]] * (rows // 128), axis=1)
            w = jnp.exp(log_sig + later)
            if first:
                w = jnp.where(before, w, 0.0)
            o = mm(w.astype(jnp.bfloat16), v)
            if first:
                acc[:, hs] = o
                carry[h] = both[:, rows:]
            else:
                acc[:, hs] += o
                carry[h] += both[:, rows:]

    block(place, True)

    @pl.loop(0, place)
    def _(step):
        block(place - 1 - step, False)

    out_ref[:, :width] = acc[...].astype(jnp.bfloat16)

    state[...] = jnp.zeros_like(state)

    def earlier(step, suffix):
        number = place - 1 - step
        state[...] += kv_ref[number, rows : rows + REC_VAL, :].astype(jnp.float32) * jnp.exp(suffix)
        tail = kv_ref[number, rows + REC_VAL :, :].astype(jnp.float32)
        return suffix + jnp.sum(tail, axis=0, keepdims=True)

    lax.fori_loop(0, place, earlier, jnp.zeros((1, state.shape[1]), jnp.float32))
    for h in range(local_ref.shape[1] // REC_VAL):
        ks = slice(h * REC_KEY, (h + 1) * REC_KEY)
        vs = slice(h * REC_VAL, (h + 1) * REC_VAL)
        raw = local_ref[:, vs] + mm(qdec_ref[:, ks], state[:, ks].astype(jnp.bfloat16), NT)
        gate = gate_ref[:, vs].astype(jnp.float32)
        mean = jnp.sum(raw * raw, axis=1, keepdims=True) * (1.0 / REC_VAL)
        done = raw * lax.rsqrt(mean + epsilon) * gain_ref[...] * (gate * jax.nn.sigmoid(gate))
        out_ref[:, width + h * REC_VAL : width + (h + 1) * REC_VAL] = done.astype(jnp.bfloat16)


def gather_kernel(planes, in_ref, out_ref, own_sem, send_sem, recv_sem):
    me = lax.axis_index("sp")
    c, y, z = lax.rem(me, 2), lax.rem(me // 2, 2), me // 4
    across, other = z * 4 + (1 - y) * 2 + c, z * 4 + y * 2 + (1 - c)
    ahead = lax.rem(z + 1, planes) * 4 + y * 2 + c
    behind = lax.rem(z + planes - 1, planes) * 4 + y * 2 + c
    barrier = pltpu.get_barrier_semaphore()
    for neighbour in (across, other, ahead, behind):
        pl.semaphore_signal(barrier, inc=1, device_id={"sp": neighbour}, device_id_type=pl.DeviceIdType.MESH)
    own = pltpu.make_async_copy(in_ref, out_ref.at[me], own_sem)
    own.start()
    pl.semaphore_wait(barrier, 4)
    own.wait()

    def copy(number, way, target):
        return pltpu.make_async_remote_copy(
            src_ref=out_ref.at[number],
            dst_ref=out_ref.at[number],
            send_sem=send_sem.at[way, number],
            recv_sem=recv_sem.at[number],
            device_id={"sp": target},
            device_id_type=pl.DeviceIdType.MESH,
        )

    def column(d):
        return (z - d) * 4 + y * 2 + c

    def facing(d):
        return (z - d) * 4 + (1 - y) * 2 + c

    def column_sends(d, act):
        @pl.when(z < planes - 1)
        def _():
            act(copy(column(d), 0, ahead))

        @pl.when((d > 0) | (y == 0))
        def _():
            act(copy(column(d), 1, across))

        @pl.when((d > 0) | (c == 0))
        def _():
            act(copy(column(d), 2, other))

    def facing_sends(d, act):
        @pl.when((d > 0) | (y == 1))
        def _():
            act(copy(facing(d), 2, other))

    def start(one):
        one.start()

    @pl.loop(0, z + 2)
    def _(d):
        @pl.when(d <= z)
        def _():
            @pl.when(d > 0)
            def _():
                copy(column(d), 0, ahead).wait_recv()

            column_sends(d, start)

        @pl.when(d > 0)
        def _():
            @pl.when((d > 1) | (y == 1))
            def _():
                copy(facing(d - 1), 1, across).wait_recv()

            facing_sends(d - 1, start)

    @pl.loop(0, z + 1)
    def _(d):
        @pl.when((d > 0) | (c == 1))
        def _():
            copy((z - d) * 4 + y * 2 + 1 - c, 2, other).wait_recv()

        @pl.when((d > 0) | (y == 1))
        def _():
            copy((z - d) * 4 + (1 - y) * 2 + 1 - c, 2, other).wait_recv()

        column_sends(d, lambda one: one.wait_send())
        facing_sends(d, lambda one: one.wait_send())


def shards(
    sp,
    tp,
    tokens,
    input_norm_gain,
    attention_query_weight,
    attention_key_weight,
    attention_value_weight,
    attention_score_bias,
    recurrence_query_weight,
    forget_weight,
    input_weight,
    output_gate_weight,
    forget_minimum,
    decay_spikes,
    head_norm_gain,
    attention_output_weight,
    recurrence_output_weight,
):
    rows = tokens.shape[0]
    mine = lax.axis_index("tp")

    def to_partner(array, shift):
        return lax.ppermute(array, "tp", [(i, (i + shift) % tp) for i in range(tp)])

    features = tokens.shape[1]
    values = jnp.zeros((rows, features * tp), tokens.dtype)
    for shift in range(tp):
        piece = tokens if shift == 0 else to_partner(tokens, shift)
        values = lax.dynamic_update_slice_in_dim(values, piece, lax.rem(mine + tp - shift, tp) * features, 1)
    attention_output_weight, recurrence_output_weight, values = lax.optimization_barrier(
        (attention_output_weight, recurrence_output_weight, values)
    )
    own_rows = jnp.concatenate([attention_output_weight, recurrence_output_weight], axis=0)
    columns = own_rows.shape[1] // tp

    def cut(shift):
        return lax.dynamic_slice_in_dim(own_rows, lax.rem(mine + shift, tp) * columns, columns, 1)

    out_weights = [cut(0)] + [to_partner(cut(shift), shift) for shift in range(1, tp)]

    values = values.astype(jnp.float32)
    scaled = (values * input_norm_gain[None, :]).astype(jnp.bfloat16)
    squares = jnp.mean(values * values, axis=1)
    inverse = lax.rsqrt(squares + epsilon)[:, None]

    def project(weight):
        return (jnp.dot(scaled, weight, preferred_element_type=jnp.float32) * inverse).astype(jnp.bfloat16)

    key_stick, value_stick = project(attention_key_weight), project(attention_value_weight)
    query_rows, forget_rows = project(recurrence_query_weight), project(forget_weight)
    input_rows = project(input_weight)
    heads_here = forget_minimum.shape[0]
    wide, narrow = heads_here * REC_KEY, heads_here * REC_VAL
    local_out, query_decayed, payload = pl.pallas_call(
        local_kernel,
        out_shape=(
            jax.ShapeDtypeStruct((rows, narrow), jnp.float32),
            jax.ShapeDtypeStruct((rows, wide), jnp.bfloat16),
            jax.ShapeDtypeStruct((rows + REC_VAL + TAIL, wide), jnp.bfloat16),
        ),
        in_specs=[VMEM] * 8,
        out_specs=(VMEM,) * 3,
        cost_estimate=pl.CostEstimate(flops=10**9, bytes_accessed=2 * 10**6, transcendentals=10**6),
        name="recurrence_local",
    )(
        key_stick,
        value_stick,
        query_rows,
        forget_rows,
        input_rows,
        forget_minimum.reshape(1, wide),
        decay_spikes,
        decay_spikes.T,
    )
    kv_all = pl.pallas_call(
        functools.partial(gather_kernel, sp // 4),
        out_shape=jax.ShapeDtypeStruct((sp,) + payload.shape, payload.dtype),
        in_specs=[VMEM],
        out_specs=VMEM,
        scratch_shapes=[
            pltpu.SemaphoreType.DMA,
            pltpu.SemaphoreType.DMA((3, sp)),
            pltpu.SemaphoreType.DMA((sp,)),
        ],
        compiler_params=pltpu.CompilerParams(collective_id=0, has_side_effects=True),
        cost_estimate=pl.CostEstimate(flops=10**10, bytes_accessed=10**8, transcendentals=0),
        name="gather_earlier",
    )(payload)
    query_stick, gate_rows = project(attention_query_weight), project(output_gate_weight)
    width = query_stick.shape[1]
    heads = pl.pallas_call(
        mix_kernel,
        out_shape=jax.ShapeDtypeStruct((rows, width + narrow), jnp.bfloat16),
        in_specs=[SMEM] + [VMEM] * 6,
        out_specs=VMEM,
        scratch_shapes=[
            pltpu.VMEM((rows, width), jnp.float32),
            pltpu.VMEM((width // HEAD, rows, 128), jnp.float32),
            pltpu.VMEM((REC_VAL, wide), jnp.float32),
        ],
        compiler_params=pltpu.CompilerParams(vmem_limit_bytes=60 * 1024 * 1024),
        name="mix_heads",
    )(
        attention_score_bias,
        query_stick,
        kv_all,
        local_out,
        query_decayed,
        gate_rows,
        head_norm_gain.reshape(1, REC_VAL),
    )
    mixed = jnp.dot(heads, out_weights[0], preferred_element_type=jnp.float32)
    for shift in range(1, tp):
        mixed = mixed + jnp.dot(to_partner(heads, shift), out_weights[shift], preferred_element_type=jnp.float32)
    return mixed.astype(jnp.bfloat16)


def solution(mesh):
    placed = (
        P("sp", "tp"),
        P(),
        P(None, "tp"),
        P(None, "tp"),
        P(None, "tp"),
        P("tp"),
        P(None, "tp"),
        P(None, "tp"),
        P(None, "tp"),
        P(None, "tp"),
        P("tp", None),
        P("sp", "tp"),
        P(),
        P("tp", None),
        P("tp", None),
    )
    return jax.shard_map(
        functools.partial(shards, mesh.shape["sp"], mesh.shape["tp"]),
        mesh=mesh,
        in_specs=placed,
        out_specs=P("sp", "tp"),
        check_vma=False,
    )
```

```python
import functools

import jax
import jax.numpy as jnp
from jax import lax
from jax.experimental import pallas as pl
from jax.experimental.pallas import tpu as pltpu
from jax.sharding import PartitionSpec as P

HEAD = 64
REC_KEY = 128
REC_VAL = 64
TAIL = 16
epsilon = 1e-06
VMEM = pl.BlockSpec(memory_space=pltpu.VMEM)
SMEM = pl.BlockSpec(memory_space=pltpu.SMEM)
NT = (((1,), (1,)), ((), ()))
TN = (((0,), (0,)), ((), ()))


def mm(a, b, dims=(((1,), (0,)), ((), ()))):
    return lax.dot_general(a, b, dims, preferred_element_type=jnp.float32)


def split(x):
    hi = x.astype(jnp.bfloat16)
    return hi, (x - hi.astype(jnp.float32)).astype(jnp.bfloat16)


def iota(shape, dim):
    return lax.broadcasted_iota(jnp.int32, shape, dim)


def local_kernel(
    key_ref, value_ref, q_ref, f_ref, v_ref, low_ref, spike_ref, spike_t_ref, out_ref, qdec_ref, pay_ref
):
    rows, width = key_ref.shape
    pay_ref[0:rows, :width] = key_ref[...]
    pay_ref[0:rows, width:] = value_ref[...]
    which = iota((TAIL, REC_KEY), 0)
    heads = v_ref.shape[1] // REC_VAL
    r, c = iota((rows, rows), 0), iota((rows, rows), 1)
    causal = r >= c
    lower = causal.astype(jnp.bfloat16)
    upper = (r <= c).astype(jnp.bfloat16)
    hi, lo = split(spike_ref[...])
    spike_col = mm(lower, hi) + mm(lower, lo)
    hi, lo = split(spike_t_ref[...])
    spike_row = mm(hi, upper) + mm(lo, upper)
    for h in range(heads):
        ks = slice(h * REC_KEY, (h + 1) * REC_KEY)
        vs = slice(h * REC_VAL, (h + 1) * REC_VAL)
        q = q_ref[:, ks].astype(jnp.float32)
        lifted = q * jax.nn.sigmoid(q)
        intake = (1.0 - low_ref[:, ks]) * jax.nn.sigmoid(-f_ref[:, ks].astype(jnp.float32))
        hi, lo = split(jnp.log1p(-intake))
        run = mm(lower, hi) + mm(lower, lo)
        s_col = spike_col[:, h : h + 1]
        s_row = spike_row[h : h + 1, :]
        q_up = lifted * jnp.exp(run)
        k_down = (intake * jnp.exp(-run)).astype(jnp.bfloat16)
        decay = jnp.exp(jnp.where(causal, s_col - s_row, 0.0))
        inner = jnp.where(causal, mm(q_up.astype(jnp.bfloat16), k_down, NT) * decay, 0.0)
        v = v_ref[:, vs]
        out_ref[:, vs] = mm(inner.astype(jnp.bfloat16), v)
        qdec_ref[:, ks] = (q_up * jnp.exp(s_col)).astype(jnp.bfloat16)
        total = run[rows - 1 : rows, :] + s_col[rows - 1 : rows, :]
        k_end = (intake * jnp.exp(total - (run + s_col))).astype(jnp.bfloat16)
        pay_ref[rows : rows + REC_VAL, ks] = mm(v, k_end, TN).astype(jnp.bfloat16)
        hi, lo = split(total)
        lo, rest = split(total - hi.astype(jnp.float32))
        tail = jnp.where(which == 0, hi.astype(jnp.float32), jnp.where(which == 1, lo.astype(jnp.float32), 0.0))
        tail = jnp.where(which == 2, rest.astype(jnp.float32), tail)
        pay_ref[rows + REC_VAL :, ks] = tail.astype(jnp.bfloat16)


def mix_kernel(bias_ref, q_ref, kv_ref, local_ref, qdec_ref, gate_ref, gain_ref, out_ref, acc, carry, state):
    rows, width = q_ref.shape
    heads = width // HEAD
    place = lax.axis_index("sp")
    r, c = iota((rows, rows), 0), iota((rows, rows), 1)
    before = c < r
    sums = jnp.concatenate(
        [(r > c).astype(jnp.bfloat16), jnp.ones((rows, 128), jnp.bfloat16)], axis=1
    )

    def block(number, first):
        for h in range(heads):
            hs = slice(h * HEAD, (h + 1) * HEAD)
            k = kv_ref[number, :rows, hs]
            v = kv_ref[number, :rows, width + h * HEAD : width + (h + 1) * HEAD]
            s = mm(q_ref[:, hs] * jnp.bfloat16(HEAD**-0.5), k, NT) + bias_ref[h]
            t = jnp.exp(-jnp.abs(s))
            soft = jnp.where(t < 3.5e-4, t, jnp.log(1.0 + t))
            log_sig = jnp.minimum(s, 0.0) - soft
            rest = log_sig - s
            if first:
                rest = jnp.where(before, rest, 0.0)
            both = mm(rest.astype(jnp.bfloat16), sums)
            later = both[:, :rows]
            if not first:
                later = later + jnp.concatenate([carry[h]] * (rows // 128), axis=1)
            w = jnp.exp(log_sig + later)
            if first:
                w = jnp.where(before, w, 0.0)
            o = mm(w.astype(jnp.bfloat16), v)
            if first:
                acc[:, hs] = o
                carry[h] = both[:, rows:]
            else:
                acc[:, hs] += o
                carry[h] += both[:, rows:]

    block(place, True)

    @pl.loop(0, place)
    def _(step):
        block(place - 1 - step, False)

    out_ref[:, :width] = acc[...].astype(jnp.bfloat16)

    state[...] = jnp.zeros_like(state)

    def earlier(step, suffix):
        number = place - 1 - step
        state[...] += kv_ref[number, rows : rows + REC_VAL, :].astype(jnp.float32) * jnp.exp(suffix)
        tail = kv_ref[number, rows + REC_VAL :, :].astype(jnp.float32)
        return suffix + jnp.sum(tail, axis=0, keepdims=True)

    lax.fori_loop(0, place, earlier, jnp.zeros((1, state.shape[1]), jnp.float32))
    for h in range(local_ref.shape[1] // REC_VAL):
        ks = slice(h * REC_KEY, (h + 1) * REC_KEY)
        vs = slice(h * REC_VAL, (h + 1) * REC_VAL)
        raw = local_ref[:, vs] + mm(qdec_ref[:, ks], state[:, ks].astype(jnp.bfloat16), NT)
        gate = gate_ref[:, vs].astype(jnp.float32)
        mean = jnp.sum(raw * raw, axis=1, keepdims=True) * (1.0 / REC_VAL)
        done = raw * lax.rsqrt(mean + epsilon) * gain_ref[...] * (gate * jax.nn.sigmoid(gate))
        out_ref[:, width + h * REC_VAL : width + (h + 1) * REC_VAL] = done.astype(jnp.bfloat16)


def gather_kernel(planes, in_ref, out_ref, own_sem, send_sem, recv_sem):
    me = lax.axis_index("sp")
    c, y, z = lax.rem(me, 2), lax.rem(me // 2, 2), me // 4
    across, other = z * 4 + (1 - y) * 2 + c, z * 4 + y * 2 + (1 - c)
    ahead = lax.rem(z + 1, planes) * 4 + y * 2 + c
    behind = lax.rem(z + planes - 1, planes) * 4 + y * 2 + c
    barrier = pltpu.get_barrier_semaphore()
    for neighbour in (across, other, ahead, behind):
        pl.semaphore_signal(barrier, inc=1, device_id={"sp": neighbour}, device_id_type=pl.DeviceIdType.MESH)
    own = pltpu.make_async_copy(in_ref, out_ref.at[me], own_sem)
    own.start()
    pl.semaphore_wait(barrier, 4)
    own.wait()

    def copy(number, way, target):
        return pltpu.make_async_remote_copy(
            src_ref=out_ref.at[number],
            dst_ref=out_ref.at[number],
            send_sem=send_sem.at[way, number],
            recv_sem=recv_sem.at[number],
            device_id={"sp": target},
            device_id_type=pl.DeviceIdType.MESH,
        )

    def column(d):
        return (z - d) * 4 + y * 2 + c

    def facing(d):
        return (z - d) * 4 + (1 - y) * 2 + c

    def column_sends(d, act):
        @pl.when(z < planes - 1)
        def _():
            act(copy(column(d), 0, ahead))

        @pl.when((d > 0) | (y == 0))
        def _():
            act(copy(column(d), 1, across))

        @pl.when((d > 0) | (c == 0))
        def _():
            act(copy(column(d), 2, other))

    def facing_sends(d, act):
        @pl.when((d > 0) | (y == 1))
        def _():
            act(copy(facing(d), 2, other))

    def start(one):
        one.start()

    @pl.loop(0, z + 2)
    def _(d):
        @pl.when(d <= z)
        def _():
            @pl.when(d > 0)
            def _():
                copy(column(d), 0, ahead).wait_recv()

            column_sends(d, start)

        @pl.when(d > 0)
        def _():
            @pl.when((d > 1) | (y == 1))
            def _():
                copy(facing(d - 1), 1, across).wait_recv()

            facing_sends(d - 1, start)

    @pl.loop(0, z + 1)
    def _(d):
        @pl.when((d > 0) | (c == 1))
        def _():
            copy((z - d) * 4 + y * 2 + 1 - c, 2, other).wait_recv()

        @pl.when((d > 0) | (y == 1))
        def _():
            copy((z - d) * 4 + (1 - y) * 2 + 1 - c, 2, other).wait_recv()

        column_sends(d, lambda one: one.wait_send())
        facing_sends(d, lambda one: one.wait_send())


def shards(
    sp,
    tp,
    tokens,
    input_norm_gain,
    attention_query_weight,
    attention_key_weight,
    attention_value_weight,
    attention_score_bias,
    recurrence_query_weight,
    forget_weight,
    input_weight,
    output_gate_weight,
    forget_minimum,
    decay_spikes,
    head_norm_gain,
    attention_output_weight,
    recurrence_output_weight,
):
    rows = tokens.shape[0]
    mine = lax.axis_index("tp")

    def to_partner(array, shift):
        return lax.ppermute(array, "tp", [(i, (i + shift) % tp) for i in range(tp)])

    features = tokens.shape[1]
    pieces = [tokens] + [to_partner(tokens, shift) for shift in range(1, tp)]
    attention_output_weight, recurrence_output_weight, pieces[-1] = lax.optimization_barrier(
        (attention_output_weight, recurrence_output_weight, pieces[-1])
    )
    own_rows = jnp.concatenate([attention_output_weight, recurrence_output_weight], axis=0)
    columns = own_rows.shape[1] // tp

    def cut(shift):
        return lax.dynamic_slice_in_dim(own_rows, lax.rem(mine + shift, tp) * columns, columns, 1)

    out_weights = [cut(0)] + [to_partner(cut(shift), shift) for shift in range(1, tp)]

    starts = [lax.rem(mine + tp - shift, tp) * features for shift in range(tp)]
    values = [piece.astype(jnp.float32) for piece in pieces]
    scaled = [
        (value * lax.dynamic_slice_in_dim(input_norm_gain, start, features, 0)[None, :]).astype(jnp.bfloat16)
        for value, start in zip(values, starts)
    ]
    squares = sum(jnp.sum(value * value, axis=1) for value in values) / (features * tp)
    inverse = lax.rsqrt(squares + epsilon)[:, None]

    def project(weight):
        total = sum(
            jnp.dot(part, lax.dynamic_slice_in_dim(weight, start, features, 0), preferred_element_type=jnp.float32)
            for part, start in zip(scaled, starts)
        )
        return (total * inverse).astype(jnp.bfloat16)

    key_stick, value_stick = project(attention_key_weight), project(attention_value_weight)
    query_rows, forget_rows = project(recurrence_query_weight), project(forget_weight)
    input_rows = project(input_weight)
    heads_here = forget_minimum.shape[0]
    wide, narrow = heads_here * REC_KEY, heads_here * REC_VAL
    local_out, query_decayed, payload = pl.pallas_call(
        local_kernel,
        out_shape=(
            jax.ShapeDtypeStruct((rows, narrow), jnp.float32),
            jax.ShapeDtypeStruct((rows, wide), jnp.bfloat16),
            jax.ShapeDtypeStruct((rows + REC_VAL + TAIL, wide), jnp.bfloat16),
        ),
        in_specs=[VMEM] * 8,
        out_specs=(VMEM,) * 3,
        cost_estimate=pl.CostEstimate(flops=10**9, bytes_accessed=2 * 10**6, transcendentals=10**6),
        name="recurrence_local",
    )(
        key_stick,
        value_stick,
        query_rows,
        forget_rows,
        input_rows,
        forget_minimum.reshape(1, wide),
        decay_spikes,
        decay_spikes.T,
    )
    kv_all = pl.pallas_call(
        functools.partial(gather_kernel, sp // 4),
        out_shape=jax.ShapeDtypeStruct((sp,) + payload.shape, payload.dtype),
        in_specs=[VMEM],
        out_specs=VMEM,
        scratch_shapes=[
            pltpu.SemaphoreType.DMA,
            pltpu.SemaphoreType.DMA((3, sp)),
            pltpu.SemaphoreType.DMA((sp,)),
        ],
        compiler_params=pltpu.CompilerParams(collective_id=0, has_side_effects=True),
        cost_estimate=pl.CostEstimate(flops=10**10, bytes_accessed=10**8, transcendentals=0),
        name="gather_earlier",
    )(payload)
    query_stick, gate_rows = project(attention_query_weight), project(output_gate_weight)
    width = query_stick.shape[1]
    heads = pl.pallas_call(
        mix_kernel,
        out_shape=jax.ShapeDtypeStruct((rows, width + narrow), jnp.bfloat16),
        in_specs=[SMEM] + [VMEM] * 6,
        out_specs=VMEM,
        scratch_shapes=[
            pltpu.VMEM((rows, width), jnp.float32),
            pltpu.VMEM((width // HEAD, rows, 128), jnp.float32),
            pltpu.VMEM((REC_VAL, wide), jnp.float32),
        ],
        compiler_params=pltpu.CompilerParams(vmem_limit_bytes=60 * 1024 * 1024),
        name="mix_heads",
    )(
        attention_score_bias,
        query_stick,
        kv_all,
        local_out,
        query_decayed,
        gate_rows,
        head_norm_gain.reshape(1, REC_VAL),
    )
    mixed = jnp.dot(heads, out_weights[0], preferred_element_type=jnp.float32)
    for shift in range(1, tp):
        mixed = mixed + jnp.dot(to_partner(heads, shift), out_weights[shift], preferred_element_type=jnp.float32)
    return mixed.astype(jnp.bfloat16)


def solution(mesh):
    placed = (
        P("sp", "tp"),
        P(),
        P(None, "tp"),
        P(None, "tp"),
        P(None, "tp"),
        P("tp"),
        P(None, "tp"),
        P(None, "tp"),
        P(None, "tp"),
        P(None, "tp"),
        P("tp", None),
        P("sp", "tp"),
        P(),
        P("tp", None),
        P("tp", None),
    )
    return jax.shard_map(
        functools.partial(shards, mesh.shape["sp"], mesh.shape["tp"]),
        mesh=mesh,
        in_specs=placed,
        out_specs=P("sp", "tp"),
        check_vma=False,
    )
```
